32 devices in a mesh: ep: 32 (over z, y, x, core).
Axes of the slice: x: 2, y: 2, z: 4, core: 2. Of those that a mesh axis runs over, the one named last changes fastest.
Arguments:
- hidden_in: bfloat16 [256, 2048], P('ep'), may hold values from -6 to 6
- w_query: bfloat16 [2048, 2048], P(None, 'ep'), may hold values from -0.125 to 0.125
- w_key: bfloat16 [2048, 256], replicated, may hold values from -0.125 to 0.125
- w_value: bfloat16 [2048, 256], replicated, may hold values from -0.125 to 0.125
- w_forget: bfloat16 [2048, 16], replicated, may hold values from -0.125 to 0.125
- w_out: bfloat16 [2048, 2048], P(None, 'ep'), may hold values from -0.125 to 0.125
- attn_gain: bfloat16 [2048], replicated, may hold values from 0.099609375 to 1.8984375
- key_cache: bfloat16 [256, 1024, 256], P('ep'), may hold values from -300 to 300
- value_cache: bfloat16 [256, 1024, 256], P('ep'), may hold values from -6 to 6
- gate_totals: float32 [256, 16, 1024], P('ep'), may hold values from -80 to 0
- lengths: int32 [256], P('ep'), may hold values from 128 to 1024, as said below
- mix_gain: bfloat16 [2048], replicated, may hold values from 0.099609375 to 1.8984375
- route_ids: int32 [256, 4], P('ep'), may hold values from 0 to 31, all different within a row; in each aligned block of 256 rows (0 to 255, 256 to 511, ...) at most 64 rows name the same one
- route_weights: float32 [256, 4], P('ep'), may hold values from 0.2 to 1
- exp_gate: bfloat16 [32, 2048, 512], P('ep'), may hold values from -0.125 to 0.125
- exp_up: bfloat16 [32, 2048, 512], P('ep'), may hold values from -0.125 to 0.125
- exp_down: bfloat16 [32, 512, 2048], P('ep'), may hold values from -0.25 to 0.25
- shared_gate: bfloat16 [2048, 512], replicated, may hold values from -0.125 to 0.125
- shared_up: bfloat16 [2048, 512], replicated, may hold values from -0.125 to 0.125
- shared_down: bfloat16 [512, 2048], replicated, may hold values from -0.25 to 0.25
- dense_gate: bfloat16 [2048, 8192], P(None, 'ep'), may hold values from -0.125 to 0.125
- dense_up: bfloat16 [2048, 8192], P(None, 'ep'), may hold values from -0.125 to 0.125
- dense_down: bfloat16 [8192, 2048], P('ep'), may hold values from -0.0625 to 0.0625
- blend_weight: bfloat16 [2048], replicated, may hold values from -0.125 to 0.125
Outputs:
- layer_out: bfloat16 [256, 2048], P('ep')
The draws below stay inside these ranges and needn't reach their ends.
Inputs may be any that keep to these rules, and one draw needn't show every extreme that they name: `lengths`: some sequence has exactly 1024 cached positions. `route_ids`: each row names 4 different experts; no expert is named by more than 64 rows in all, and some expert by exactly that many.
All inputs are finite; a program needn't handle non-finite values.
Results may differ from the reference program's by a relative error of at most 0.015.
Values may be sent and summed in bfloat16 or wider, within the bound.
No kernel may reach another device: no remote copies, remote signals or barrier semaphores. Data moves between devices by JAX's collectives and lax.ppermute only.
A program may use at most 128 MiB of HBM per device.

```python
import math
import jax
import jax.numpy as jnp
import numpy as np
from jax import lax

D = 2048
HEADS = 16
HEAD_DIM = 128
KV_HEADS = 2
CACHE_SLOTS = 1024
TOK_DEV = 8
EXPERT_FF = 512
SHARED_FF = 512
DENSE_FF = 8192
TOPK = 4
EXPERTS = 32
TOKEN_COUNT = 256
CAPACITY = 64


def draw_key_cache(key, part):
    base = jnp.clip(jax.random.normal(key, (TOKEN_COUNT, CACHE_SLOTS, KV_HEADS * HEAD_DIM), jnp.float32), -4.5, 4.5)
    return base.astype(jnp.bfloat16)


def draw_gate_totals(key, part):
    order = jax.random.permutation(jax.random.fold_in(key, 1), HEADS)
    slow_heads = order < HEADS // 2
    factor = jnp.exp(jax.random.uniform(jax.random.fold_in(key, 2), (TOKEN_COUNT, 1, 1), jnp.float32, 0.0, 1.0986))
    rough = jax.random.uniform(jax.random.fold_in(key, 3), (TOKEN_COUNT, HEADS, CACHE_SLOTS), jnp.float32, 0.5, 1.5)
    rates = jnp.where(slow_heads, 0.25 / CACHE_SLOTS, 0.015).astype(jnp.float32)[None, :, None] * factor
    decode_steps = -rates * rough
    spike_position = jax.random.randint(jax.random.fold_in(key, 4), (TOKEN_COUNT, 2), 0, CACHE_SLOTS)
    spike_penalty = jax.random.uniform(jax.random.fold_in(key, 5), (TOKEN_COUNT, 2), jnp.float32, -0.69, -0.22)
    token_positions = jnp.arange(CACHE_SLOTS, dtype=jnp.int32)
    match_total = (token_positions[None, None, :] == spike_position[:, :, None]).astype(jnp.float32)
    spike_events = jnp.sum(match_total * spike_penalty[:, :, None], axis=1)
    decode_steps = decode_steps + spike_events[:, None, :]
    return jnp.cumsum(decode_steps, axis=2)


def draw_lengths(key, part):
    block_count = TOKEN_COUNT // TOK_DEV
    device_top = jax.random.randint(jax.random.fold_in(key, 1), (block_count, 1), CACHE_SLOTS // 4, CACHE_SLOTS + 1)
    lens = jax.random.randint(jax.random.fold_in(key, 2), (block_count, TOK_DEV), CACHE_SLOTS // 8, device_top + 1).reshape(TOKEN_COUNT)
    chosen = jax.random.randint(jax.random.fold_in(key, 3), (), 0, TOKEN_COUNT)
    return jnp.where(jnp.arange(TOKEN_COUNT, dtype=jnp.int32) == chosen, CACHE_SLOTS, lens).astype(jnp.int32)


def steps_of(key, dims, pieces, low, high):
    level = 1.0
    for position, shards_of in pieces:
        heights = jax.random.uniform(jax.random.fold_in(jax.random.fold_in(key, 6), position), (shards_of,), jnp.float32, low / len(pieces), high / len(pieces))
        level = level * jnp.repeat(jnp.exp(heights), dims[position] // shards_of).reshape((-1,) + (1,) * (len(dims) - 1 - position))
    return level


def deal_out(stream_key, own, number, rows, number_of, top, bound, lean):
    order = jax.random.permutation(stream_key, number_of)
    heavy_load, ordinary = load_shares(number_of, rows * top, bound, lean, True), load_shares(number_of, rows * top, bound, lean, False)
    places = jnp.arange(number_of)

    def named(sizes, turn):
        used = int((sizes > 0).sum())
        fixed = max(1, used // 4)
        moved = fixed + (places - fixed + turn * (used - fixed)) % max(1, number_of - fixed)
        return jnp.zeros((number_of,), jnp.int32).at[order[jnp.where(places < fixed, places, moved)]].set(jnp.asarray(sizes, jnp.int32))

    sizes = jnp.where(number % 4 == 0, named(heavy_load, number // 4), named(ordinary, number - number // 4 - 1))
    mixed = jax.random.permutation(jax.random.fold_in(own, 3), number_of)
    source_of, taker = mixed[0:number_of // 2 * 2:2], mixed[1:number_of // 2 * 2:2]
    room = jnp.minimum(sizes[source_of] - 1, bound - sizes[taker]) // 2
    room = jnp.where((source_of == order[0]) | (taker == order[0]) | (sizes[taker] == 0), 0, jnp.maximum(room, 0))
    moved = jax.random.randint(jax.random.fold_in(own, 4), (number_of // 2,), 0, 1 << 20) % (room + 1)
    sizes = sizes.at[source_of].add(-moved).at[taker].add(moved)
    members = jnp.searchsorted(jnp.cumsum(sizes), jnp.arange(rows * top), side="right").astype(jnp.int32)
    table = members.reshape(top, rows).T
    table = table[jax.random.permutation(jax.random.fold_in(own, 1), rows)]
    turn = jax.random.randint(jax.random.fold_in(own, 2), (rows, 1), 0, top)
    return jnp.take_along_axis(table, (jnp.arange(top)[None, :] + turn) % top, axis=1)


def load_shares(amount, total, most, lean, full):
    weights = [(1 << 20) // math.isqrt(rank ** lean) + 1 for rank in range(1, amount + 1)]
    largest = most if full else min(most, max(-(-total // amount), total * weights[0] // sum(weights)))
    least = 1 if total - largest >= amount - 1 else 0
    counts, spare = [largest] + [least] * (amount - 1), total - largest - least * (amount - 1)
    while spare > 0:
        candidates = [i for i in range(1, amount) if counts[i] < largest] or [i for i in range(1, amount) if counts[i] < most]
        mass, left = sum([weights[i] for i in candidates]), spare
        for i in candidates:
            extra = min(most - counts[i], max(1, left * weights[i] // mass), spare)
            counts[i] = counts[i] + extra
            spare = spare - extra
    return np.array(counts)


def scatter_about(rng, dims, scale, reach, cuts=(), held_as=jnp.bfloat16):
    result = scale * jax.random.normal(rng, dims, jnp.float32)
    if cuts:
        result = result * steps_of(rng, dims, cuts, -0.22, 0.18)
    return jnp.clip(result, -reach, reach).astype(held_as)


def setup_inputs(seed: int = 0) -> dict:
    splits = jax.random.split(jax.random.key(seed), 25)
    hidden_in = scatter_about(splits[0], (TOKEN_COUNT, D), 1.0, 6.0, ((0, 32),))
    w_query = scatter_about(splits[1], (D, HEADS * HEAD_DIM), D ** -0.5, 0.125, ((1, 32),))
    w_key = scatter_about(splits[2], (D, KV_HEADS * HEAD_DIM), D ** -0.5, 0.125)
    w_value = scatter_about(splits[3], (D, KV_HEADS * HEAD_DIM), D ** -0.5, 0.125)
    w_forget = scatter_about(splits[4], (D, HEADS), D ** -0.5, 0.125)
    w_out = scatter_about(splits[5], (HEADS * HEAD_DIM, D), (HEADS * HEAD_DIM) ** -0.5, 0.125, ((1, 32),))
    attn_gain = jnp.clip(1.0 + 0.18 * jax.random.normal(splits[6], (D,), jnp.float32), 0.099609375, 1.8984375).astype(jnp.bfloat16)
    key_cache = draw_key_cache(jax.random.fold_in(splits[24], 71), 0)
    value_cache = scatter_about(splits[8], (TOKEN_COUNT, CACHE_SLOTS, KV_HEADS * HEAD_DIM), 1.0, 6.0, ((0, 32),))
    gate_totals = draw_gate_totals(jax.random.fold_in(splits[24], 71), 0)
    lengths = draw_lengths(jax.random.fold_in(splits[24], 71), 0)
    mix_gain = jnp.clip(1.0 + 0.18 * jax.random.normal(splits[11], (D,), jnp.float32), 0.099609375, 1.8984375).astype(jnp.bfloat16)
    route_ids_keys = jax.random.split(jax.random.fold_in(splits[12], 1), TOKEN_COUNT // TOKEN_COUNT)
    route_ids_turns = jax.random.permutation(jax.random.fold_in(splits[12], 3), TOKEN_COUNT // TOKEN_COUNT)
    route_ids = jax.vmap(lambda own, number: deal_out(jax.random.fold_in(splits[12], 2), own, number, TOKEN_COUNT, EXPERTS, TOPK, CAPACITY, 2))(route_ids_keys, route_ids_turns).reshape((TOKEN_COUNT, TOPK))
    route_weights = jnp.clip(jnp.exp(math.log(1.0) - 1.609438 * jax.random.uniform(splits[13], (TOKEN_COUNT, TOPK), jnp.float32) ** steps_of(splits[13], (TOKEN_COUNT, TOPK), ((0, 32),), -0.2, 0.2)), 0.2, 1.0)
    exp_gate = scatter_about(splits[14], (EXPERTS, D, EXPERT_FF), D ** -0.5, 0.125, ((0, 32),))
    exp_up = scatter_about(splits[15], (EXPERTS, D, EXPERT_FF), D ** -0.5, 0.125, ((0, 32),))
    exp_down = scatter_about(splits[16], (EXPERTS, EXPERT_FF, D), EXPERT_FF ** -0.5, 0.25, ((0, 32),))
    shared_gate = scatter_about(splits[17], (D, SHARED_FF), D ** -0.5, 0.125)
    shared_up = scatter_about(splits[18], (D, SHARED_FF), D ** -0.5, 0.125)
    shared_down = scatter_about(splits[19], (SHARED_FF, D), SHARED_FF ** -0.5, 0.25)
    dense_gate = scatter_about(splits[20], (D, DENSE_FF), D ** -0.5, 0.125, ((1, 32),))
    dense_up = scatter_about(splits[21], (D, DENSE_FF), D ** -0.5, 0.125, ((1, 32),))
    dense_down = scatter_about(splits[22], (DENSE_FF, D), DENSE_FF ** -0.5, 0.0625, ((0, 32),))
    blend_weight = scatter_about(splits[23], (D,), D ** -0.5, 0.125)
    return dict(hidden_in=hidden_in, w_query=w_query, w_key=w_key, w_value=w_value, w_forget=w_forget, w_out=w_out, attn_gain=attn_gain, key_cache=key_cache, value_cache=value_cache, gate_totals=gate_totals, lengths=lengths, mix_gain=mix_gain, route_ids=route_ids, route_weights=route_weights, exp_gate=exp_gate, exp_up=exp_up, exp_down=exp_down, shared_gate=shared_gate, shared_up=shared_up, shared_down=shared_down, dense_gate=dense_gate, dense_up=dense_up, dense_down=dense_down, blend_weight=blend_weight)


def normalize(inputs, gain_vec):
    as_float = inputs.astype(jnp.float32)
    scaled = as_float * lax.rsqrt(lax.optimization_barrier(jnp.mean(as_float * as_float, axis=-1, keepdims=True)) + 1e-06)
    return (scaled * gain_vec.astype(jnp.float32)).astype(jnp.bfloat16)

def attend(queries, new_key, new_value, forget, key_cache, value_cache, gate_totals, lengths):
    seq_count = queries.shape[0]
    head_count = gate_totals.shape[1]
    cache_len = key_cache.shape[1]
    kv_heads = key_cache.shape[2] // HEAD_DIM
    group_size = head_count // kv_heads
    scale = HEAD_DIM ** (-0.5)
    grouped = queries.astype(jnp.float32).reshape(seq_count, kv_heads, group_size, HEAD_DIM)
    key_rows = key_cache.astype(jnp.float32).reshape(seq_count, cache_len, kv_heads, HEAD_DIM)
    scores = jnp.einsum('bgrd,bsgd->bgrs', grouped, key_rows).reshape(seq_count, head_count, cache_len) * scale
    last_pos = jnp.broadcast_to((lengths - 1).astype(jnp.int32)[:, None, None], (seq_count, head_count, 1))
    newest = jnp.take_along_axis(gate_totals, last_pos, axis=2)
    scores = scores + forget[:, :, None] + newest - gate_totals
    usable = jnp.arange(cache_len, dtype=jnp.int32)[None, None, :] < lengths[:, None, None]
    scores = jnp.where(usable, scores, -jnp.inf)
    own_score = jnp.einsum('bgrd,bgd->bgr', grouped, new_key.astype(jnp.float32).reshape(seq_count, kv_heads, HEAD_DIM))
    own_score = own_score.reshape(seq_count, head_count) * scale
    row_peak = jnp.maximum(lax.optimization_barrier(jnp.max(scores, axis=-1)), own_score)
    raised = jnp.exp(scores - row_peak[:, :, None])
    own_exp = jnp.exp(own_score - row_peak)
    row_sum = lax.optimization_barrier(jnp.sum(raised, axis=-1)) + own_exp
    probs = (raised / row_sum[:, :, None]).astype(jnp.bfloat16)
    own_prob = (own_exp / row_sum).astype(jnp.bfloat16)
    value_rows = value_cache.astype(jnp.float32).reshape(seq_count, cache_len, kv_heads, HEAD_DIM)
    blended = jnp.einsum('bgrs,bsgd->bgrd', probs.astype(jnp.float32).reshape(seq_count, kv_heads, group_size, cache_len), value_rows)
    blended = blended + own_prob.astype(jnp.float32).reshape(seq_count, kv_heads, group_size, 1) * new_value.astype(jnp.float32).reshape(seq_count, kv_heads, 1, HEAD_DIM)
    return blended.reshape(seq_count, head_count * HEAD_DIM).astype(jnp.bfloat16)

def reference(hidden_in, w_query, w_key, w_value, w_forget, w_out, attn_gain, key_cache, value_cache, gate_totals, lengths, mix_gain, route_ids, route_weights, exp_gate, exp_up, exp_down, shared_gate, shared_up, shared_down, dense_gate, dense_up, dense_down, blend_weight):
    normed = normalize(hidden_in, attn_gain)
    queries = jnp.dot(normed, w_query, preferred_element_type=jnp.float32).astype(jnp.bfloat16)
    new_key = jnp.dot(normed, w_key, preferred_element_type=jnp.float32).astype(jnp.bfloat16)
    new_value = jnp.dot(normed, w_value, preferred_element_type=jnp.float32).astype(jnp.bfloat16)
    forget = jax.nn.log_sigmoid(jnp.dot(normed, w_forget, preferred_element_type=jnp.float32))
    block_count = TOKEN_COUNT // TOK_DEV

    def split_blocks(source):
        return source.reshape((block_count, TOK_DEV) + source.shape[1:])

    def attend_block(packed):
        return attend(*packed)
    mixture = lax.map(attend_block, tuple((split_blocks(source) for source in (queries, new_key, new_value, forget, key_cache, value_cache, gate_totals, lengths))))
    mixture = mixture.reshape(TOKEN_COUNT, HEADS * HEAD_DIM)
    attn_out = jnp.dot(mixture, w_out, preferred_element_type=jnp.float32).astype(jnp.bfloat16)
    resid = (hidden_in.astype(jnp.float32) + attn_out.astype(jnp.float32)).astype(jnp.bfloat16)
    normed2 = normalize(resid, mix_gain)
    shared_hidden = (jax.nn.silu(jnp.dot(normed2, shared_gate, preferred_element_type=jnp.float32)) * jnp.dot(normed2, shared_up, preferred_element_type=jnp.float32)).astype(jnp.bfloat16)
    shared_out = jnp.dot(shared_hidden, shared_down, preferred_element_type=jnp.float32)
    blend = jax.nn.sigmoid(jnp.dot(normed2, blend_weight, preferred_element_type=jnp.float32))
    dense_hidden = (jax.nn.silu(jnp.dot(normed2, dense_gate, preferred_element_type=jnp.float32)) * jnp.dot(normed2, dense_up, preferred_element_type=jnp.float32) * blend[:, None]).astype(jnp.bfloat16)
    dense_out = jnp.dot(dense_hidden, dense_down, preferred_element_type=jnp.float32)
    expert_ids = jnp.arange(EXPERTS, dtype=jnp.int32)
    coeff = lax.optimization_barrier(jnp.sum(jnp.where(route_ids[:, :, None] == expert_ids[None, None, :], route_weights[:, :, None], 0.0), axis=1))
    slot_ids = jnp.arange(CAPACITY, dtype=jnp.int32)

    def one_expert(carry, packed):
        gate_w, up_w, down_w, coeffs = packed
        routed = coeffs > 0
        slot_rank = jnp.cumsum(routed.astype(jnp.int32)) - 1
        dispatch = ((slot_rank[None, :] == slot_ids[:, None]) & routed[None, :]).astype(jnp.float32)
        expert_rows = jnp.dot(dispatch.astype(jnp.bfloat16), normed2, preferred_element_type=jnp.float32).astype(jnp.bfloat16)
        gate_act = jnp.dot(expert_rows, gate_w, preferred_element_type=jnp.float32)
        up_act = jnp.dot(expert_rows, up_w, preferred_element_type=jnp.float32)
        expert_hidden = (jax.nn.silu(gate_act) * up_act).astype(jnp.bfloat16)
        expert_out = jnp.dot(expert_hidden, down_w, preferred_element_type=jnp.float32).astype(jnp.bfloat16)
        weighted = dispatch * coeffs[None, :]
        carry = carry + jnp.dot(weighted.T, expert_out.astype(jnp.float32), precision=lax.Precision.HIGHEST)
        return (carry, None)
    routed_sum, unused = lax.scan(one_expert, jnp.zeros((TOKEN_COUNT, D), jnp.float32), (exp_gate, exp_up, exp_down, coeff.T))
    branch = dense_out + routed_sum
    return (resid.astype(jnp.float32) + shared_out + branch).astype(jnp.bfloat16)
```

```python
import jax
import jax.numpy as jnp
from jax import lax
from jax.sharding import PartitionSpec as P

HEAD_DIM = 128
AXIS = "ep"


def stages_of(mesh):
    count = mesh.shape[AXIS]
    sizes = []
    devices = list(mesh.devices.reshape(-1))
    if all(getattr(dev, "coords", None) is not None for dev in devices):
        for dim in (2, 1, 0):
            sizes.append(len({dev.coords[dim] for dev in devices}))
        sizes.append(len({dev.core_on_chip for dev in devices}))
    total = 1
    for size in sizes:
        total *= size
    if total != count or any(size & (size - 1) for size in sizes):
        sizes = []
        while count > 1:
            sizes.append(2)
            count //= 2
    groups = []
    stride = mesh.shape[AXIS]
    for size in sizes:
        stride //= size
        if size > 1:
            groups.append([stride * step for step in range(1, size)])
    return groups


def swap(values, mask, count):
    return lax.ppermute(values, AXIS, [(dev, dev ^ mask) for dev in range(count)])


def gather_rows(rows, groups, count):
    for group in groups:
        parts = [rows] + [swap(rows, mask, count) for mask in group]
        rows = jnp.concatenate(parts, axis=0)
    return rows


def block_order(groups):
    order = [0]
    for group in groups:
        order = order + [mask ^ prior for mask in group for prior in order]
    return order


def scatter_sum(partial, groups, count):
    for group in reversed(groups):
        size = len(group) + 1
        parts = jnp.split(partial, size, axis=0)
        total = parts[0].astype(jnp.float32)
        for mask, part in zip(group, parts[1:]):
            total = total + swap(part.astype(jnp.bfloat16), mask, count).astype(jnp.float32)
        partial = total
    return partial


def normalize(inputs, gain_vec):
    as_float = inputs.astype(jnp.float32)
    scaled = as_float * lax.rsqrt(jnp.mean(as_float * as_float, axis=-1, keepdims=True) + 1e-06)
    return (scaled * gain_vec.astype(jnp.float32)).astype(jnp.bfloat16)


def attend(queries, new_key, new_value, forget, key_cache, value_cache, gate_totals, lengths):
    seq_count = queries.shape[0]
    head_count = gate_totals.shape[1]
    cache_len = key_cache.shape[1]
    kv_heads = key_cache.shape[2] // HEAD_DIM
    group_size = head_count // kv_heads
    scale = HEAD_DIM ** (-0.5)
    grouped = queries.reshape(seq_count, kv_heads, group_size, HEAD_DIM)
    key_rows = key_cache.reshape(seq_count, cache_len, kv_heads, HEAD_DIM)
    scores = (
        jnp.einsum(
            "bgrd,bsgd->bgrs", grouped, key_rows, preferred_element_type=jnp.float32
        ).reshape(seq_count, head_count, cache_len)
        * scale
    )
    last_pos = jnp.broadcast_to((lengths - 1)[:, None, None], (seq_count, head_count, 1))
    newest = jnp.take_along_axis(gate_totals, last_pos, axis=2)
    scores = scores + forget[:, :, None] + newest - gate_totals
    usable = jnp.arange(cache_len, dtype=jnp.int32)[None, None, :] < lengths[:, None, None]
    scores = jnp.where(usable, scores, -jnp.inf)
    own_score = jnp.einsum(
        "bgrd,bgd->bgr",
        grouped,
        new_key.reshape(seq_count, kv_heads, HEAD_DIM),
        preferred_element_type=jnp.float32,
    )
    own_score = own_score.reshape(seq_count, head_count) * scale
    row_peak = jnp.maximum(jnp.max(scores, axis=-1), own_score)
    raised = jnp.exp(scores - row_peak[:, :, None])
    own_exp = jnp.exp(own_score - row_peak)
    row_sum = jnp.sum(raised, axis=-1) + own_exp
    probs = (raised / row_sum[:, :, None]).astype(jnp.bfloat16)
    own_prob = (own_exp / row_sum).astype(jnp.bfloat16)
    value_rows = value_cache.reshape(seq_count, cache_len, kv_heads, HEAD_DIM)
    blended = jnp.einsum(
        "bgrs,bsgd->bgrd",
        probs.reshape(seq_count, kv_heads, group_size, cache_len),
        value_rows,
        preferred_element_type=jnp.float32,
    )
    blended = blended + own_prob.astype(jnp.float32).reshape(
        seq_count, kv_heads, group_size, 1
    ) * new_value.astype(jnp.float32).reshape(seq_count, kv_heads, 1, HEAD_DIM)
    return blended.reshape(seq_count, head_count * HEAD_DIM).astype(jnp.bfloat16)


def keep_bf16(values):
    return lax.reduce_precision(values, exponent_bits=8, mantissa_bits=7)


def pack_routes(route_ids, route_weights, width):
    first = keep_bf16(route_weights)
    second = keep_bf16(route_weights - first)
    third = route_weights - first - second
    high = route_ids // 256
    low = route_ids % 256
    columns = [high.astype(jnp.float32), low.astype(jnp.float32), first, second, third]
    packed = jnp.concatenate(columns, axis=1).astype(jnp.bfloat16)
    return jnp.pad(packed, ((0, 0), (0, width - packed.shape[1])))


def unpack_routes(packed, topk):
    wide = packed[:, : 5 * topk].astype(jnp.float32).reshape(packed.shape[0], 5, topk)
    ids = (wide[:, 0] * 256.0 + wide[:, 1]).astype(jnp.int32)
    return ids, wide[:, 2] + wide[:, 3] + wide[:, 4]


def make_body(mesh):
    count = mesh.shape[AXIS]
    groups = stages_of(mesh)
    order = jnp.array(block_order(groups), jnp.int32)

    def on_device(
        hidden_in,
        w_query,
        w_key,
        w_value,
        w_forget,
        w_out,
        attn_gain,
        key_cache,
        value_cache,
        gate_totals,
        lengths,
        mix_gain,
        route_ids,
        route_weights,
        exp_gate,
        exp_up,
        exp_down,
        shared_gate,
        shared_up,
        shared_down,
        dense_gate,
        dense_up,
        dense_down,
        blend_weight,
    ):
        me = lax.axis_index(AXIS)
        own_rows, width = hidden_in.shape
        rows = own_rows * count
        topk = route_ids.shape[1]
        source = jnp.repeat(order ^ me, own_rows) * own_rows + jnp.tile(
            jnp.arange(own_rows, dtype=jnp.int32), count
        )
        to_device = (jnp.arange(rows, dtype=jnp.int32)[:, None] == source[None, :]).astype(
            jnp.bfloat16
        )

        def columns_of(all_rows, weights):
            cols = jnp.dot(all_rows, weights, preferred_element_type=jnp.float32)
            cols = cols.astype(jnp.bfloat16)
            sorted_cols = jnp.dot(to_device, cols, preferred_element_type=jnp.float32)
            return lax.all_to_all(
                sorted_cols.astype(jnp.bfloat16), AXIS, split_axis=0, concat_axis=1, tiled=True
            )

        normed = normalize(hidden_in, attn_gain)
        packed = pack_routes(route_ids, route_weights, 128)
        first = gather_rows(jnp.concatenate([normed, packed], axis=1), groups, count)
        ids, weights = unpack_routes(first[:, width:], topk)
        queries = columns_of(first[:, :width], w_query)
        new_key = jnp.dot(normed, w_key, preferred_element_type=jnp.float32).astype(jnp.bfloat16)
        new_value = jnp.dot(normed, w_value, preferred_element_type=jnp.float32).astype(
            jnp.bfloat16
        )
        forget = jax.nn.log_sigmoid(jnp.dot(normed, w_forget, preferred_element_type=jnp.float32))
        mixture = attend(
            queries, new_key, new_value, forget, key_cache, value_cache, gate_totals, lengths
        )
        attn_out = columns_of(gather_rows(mixture, groups, count), w_out)
        resid = (hidden_in.astype(jnp.float32) + attn_out.astype(jnp.float32)).astype(jnp.bfloat16)
        normed2 = normalize(resid, mix_gain)
        all_rows = gather_rows(normed2, groups, count)

        local = exp_gate.shape[0]
        blend = jax.nn.sigmoid(jnp.dot(all_rows, blend_weight, preferred_element_type=jnp.float32))
        dense_hidden = (
            jax.nn.silu(jnp.dot(all_rows, dense_gate, preferred_element_type=jnp.float32))
            * jnp.dot(all_rows, dense_up, preferred_element_type=jnp.float32)
            * blend[:, None]
        ).astype(jnp.bfloat16)
        partial = jnp.dot(dense_hidden, dense_down, preferred_element_type=jnp.float32)
        for j in range(local):
            coeff = jnp.sum(jnp.where(ids == me * local + j, weights, 0.0), axis=1)
            expert_hidden = (
                jax.nn.silu(jnp.dot(all_rows, exp_gate[j], preferred_element_type=jnp.float32))
                * jnp.dot(all_rows, exp_up[j], preferred_element_type=jnp.float32)
                * coeff[:, None]
            ).astype(jnp.bfloat16)
            partial = partial + jnp.dot(
                expert_hidden, exp_down[j], preferred_element_type=jnp.float32
            )
        branch = scatter_sum(partial, groups, count)
        shared_hidden = (
            jax.nn.silu(jnp.dot(normed2, shared_gate, preferred_element_type=jnp.float32))
            * jnp.dot(normed2, shared_up, preferred_element_type=jnp.float32)
        ).astype(jnp.bfloat16)
        shared_out = jnp.dot(shared_hidden, shared_down, preferred_element_type=jnp.float32)
        return (resid.astype(jnp.float32) + shared_out + branch).astype(jnp.bfloat16)

    return on_device


def solution(mesh):
    row, col, cube, whole = P(AXIS, None), P(None, AXIS), P(AXIS, None, None), P()
    placed = (
        row,
        col,
        whole,
        whole,
        whole,
        col,
        whole,
        cube,
        cube,
        cube,
        P(AXIS),
        whole,
        row,
        row,
        cube,
        cube,
        cube,
        whole,
        whole,
        whole,
        col,
        col,
        row,
        whole,
    )
    return jax.shard_map(
        make_body(mesh), mesh=mesh, in_specs=placed, out_specs=row, check_vma=False
    )
```

```python
import jax
import jax.numpy as jnp
from jax import lax
from jax.experimental import pallas as pl
from jax.experimental.pallas import tpu as pltpu
from jax.sharding import PartitionSpec as P

HEAD_DIM = 128
LANES = 128
AXIS = "ep"


def stages_of(mesh):
    count = mesh.shape[AXIS]
    sizes = []
    devices = list(mesh.devices.reshape(-1))
    if all(getattr(dev, "coords", None) is not None for dev in devices):
        for dim in (2, 1, 0):
            sizes.append(len({dev.coords[dim] for dev in devices}))
        sizes.append(len({dev.core_on_chip for dev in devices}))
    total = 1
    for size in sizes:
        total *= size
    if total != count or any(size & (size - 1) for size in sizes):
        sizes = []
        while count > 1:
            sizes.append(2)
            count //= 2
    groups = []
    stride = mesh.shape[AXIS]
    for size in sizes:
        stride //= size
        if size > 1:
            groups.append([stride * step for step in range(1, size)])
    return groups


def swap(values, mask, count):
    return lax.ppermute(values, AXIS, [(dev, dev ^ mask) for dev in range(count)])


def gather_rows(rows, groups, count):
    for group in groups:
        parts = [rows] + [swap(rows, mask, count) for mask in group]
        rows = jnp.concatenate(parts, axis=0)
    return rows


def block_order(groups):
    order = [0]
    for group in groups:
        order = order + [mask ^ prior for mask in group for prior in order]
    return order


def scatter_sum(partial, groups, count):
    for group in reversed(groups):
        size = len(group) + 1
        parts = jnp.split(partial, size, axis=0)
        total = parts[0].astype(jnp.float32)
        for mask, part in zip(group, parts[1:]):
            total = total + swap(part.astype(jnp.bfloat16), mask, count).astype(jnp.float32)
        partial = total
    return partial


def normalize(inputs, gain_vec):
    as_float = inputs.astype(jnp.float32)
    scaled = as_float * lax.rsqrt(jnp.mean(as_float * as_float, axis=-1, keepdims=True) + 1e-06)
    return (scaled * gain_vec.astype(jnp.float32)).astype(jnp.bfloat16)


def attend(queries, new_key, new_value, forget, key_cache, value_cache, gate_totals, lengths):
    seq_count = queries.shape[0]
    head_count = gate_totals.shape[1]
    cache_len = key_cache.shape[1]
    kv_heads = key_cache.shape[2] // HEAD_DIM
    group_size = head_count // kv_heads
    scale = HEAD_DIM ** (-0.5)
    grouped = queries.reshape(seq_count, kv_heads, group_size, HEAD_DIM)
    key_rows = key_cache.reshape(seq_count, cache_len, kv_heads, HEAD_DIM)
    scores = (
        jnp.einsum(
            "bgrd,bsgd->bgrs", grouped, key_rows, preferred_element_type=jnp.float32
        ).reshape(seq_count, head_count, cache_len)
        * scale
    )
    last_pos = jnp.broadcast_to((lengths - 1)[:, None, None], (seq_count, head_count, 1))
    newest = jnp.take_along_axis(gate_totals, last_pos, axis=2)
    scores = scores + forget[:, :, None] + newest - gate_totals
    usable = jnp.arange(cache_len, dtype=jnp.int32)[None, None, :] < lengths[:, None, None]
    scores = jnp.where(usable, scores, -jnp.inf)
    own_score = jnp.einsum(
        "bgrd,bgd->bgr",
        grouped,
        new_key.reshape(seq_count, kv_heads, HEAD_DIM),
        preferred_element_type=jnp.float32,
    )
    own_score = own_score.reshape(seq_count, head_count) * scale
    row_peak = jnp.maximum(jnp.max(scores, axis=-1), own_score)
    raised = jnp.exp(scores - row_peak[:, :, None])
    own_exp = jnp.exp(own_score - row_peak)
    row_sum = jnp.sum(raised, axis=-1) + own_exp
    probs = (raised / row_sum[:, :, None]).astype(jnp.bfloat16)
    own_prob = (own_exp / row_sum).astype(jnp.bfloat16)
    value_rows = value_cache.reshape(seq_count, cache_len, kv_heads, HEAD_DIM)
    blended = jnp.einsum(
        "bgrs,bsgd->bgrd",
        probs.reshape(seq_count, kv_heads, group_size, cache_len),
        value_rows,
        preferred_element_type=jnp.float32,
    )
    blended = blended + own_prob.astype(jnp.float32).reshape(
        seq_count, kv_heads, group_size, 1
    ) * new_value.astype(jnp.float32).reshape(seq_count, kv_heads, 1, HEAD_DIM)
    return blended.reshape(seq_count, head_count * HEAD_DIM).astype(jnp.bfloat16)


def keep_bf16(values):
    return lax.reduce_precision(values, exponent_bits=8, mantissa_bits=7)


def pack_routes(route_ids, route_weights, width):
    first = keep_bf16(route_weights)
    second = keep_bf16(route_weights - first)
    third = route_weights - first - second
    high = route_ids // 256
    low = route_ids % 256
    columns = [high.astype(jnp.float32), low.astype(jnp.float32), first, second, third]
    packed = jnp.concatenate(columns, axis=1).astype(jnp.bfloat16)
    return jnp.pad(packed, ((0, 0), (0, width - packed.shape[1])))


def unpack_routes(packed, topk):
    wide = packed[:, : 5 * topk].astype(jnp.float32).reshape(packed.shape[0], 5, topk)
    ids = (wide[:, 0] * 256.0 + wide[:, 1]).astype(jnp.int32)
    return ids, wide[:, 2] + wide[:, 3] + wide[:, 4]


VMEM_SPEC = pl.BlockSpec(memory_space=pltpu.VMEM)
SMEM_SPEC = pl.BlockSpec(memory_space=pltpu.SMEM)
MIB = 1024 * 1024


def across(rows, weights):
    return lax.dot_general(
        rows, weights, (((1,), (1,)), ((), ())), preferred_element_type=jnp.float32
    )


def call(kernel, name, limit, in_specs, out_shape, scratch, *args):
    result = pl.pallas_call(
        kernel,
        name=name,
        in_specs=in_specs,
        out_specs=jax.tree.map(lambda _: VMEM_SPEC, out_shape),
        out_shape=out_shape,
        scratch_shapes=scratch,
        compiler_params=pltpu.CompilerParams(vmem_limit_bytes=limit * MIB),
    )(*args)
    return list(result) if isinstance(out_shape, list) else result


def join_rows(parts):
    rows, width = parts[0].shape

    def kernel(*refs):
        for k, ref in enumerate(refs[:-1]):
            refs[-1][k * rows : (k + 1) * rows, :] = ref[...]

    return call(
        kernel,
        "join_rows",
        4,
        [VMEM_SPEC] * len(parts),
        jax.ShapeDtypeStruct((len(parts) * rows, width), parts[0].dtype),
        [],
        *parts,
    )


def chip_weights(me, own_w, other_w):
    half, width = own_w.shape

    def kernel(me_ref, own_ref, other_ref, out_ref):
        core = me_ref[0] % 2
        out_ref[pl.ds(pl.multiple_of(core * half, half), half), :] = own_ref[...]
        out_ref[pl.ds(pl.multiple_of((1 - core) * half, half), half), :] = other_ref[...]

    return call(
        kernel,
        "chip_weights",
        4,
        [SMEM_SPEC, VMEM_SPEC, VMEM_SPEC],
        jax.ShapeDtypeStruct((2 * half, width), own_w.dtype),
        [],
        me,
        own_w,
        other_w,
    )


def regroup(pieces):
    parts = len(pieces)
    blocks, rows, width = pieces[0].shape

    def kernel(*refs):
        for i in range(parts):
            for j in range(blocks):
                refs[parts + j][i] = refs[i][j]

    shape = jax.ShapeDtypeStruct((parts, rows, width), pieces[0].dtype)
    return call(kernel, "regroup", 4, [VMEM_SPEC] * parts, [shape] * blocks, [], *pieces)


def small_table(attn_gain, mix_gain, blend_weight, route_ids, route_weights):
    wide = jnp.float32
    vectors = jnp.stack([attn_gain, mix_gain, blend_weight]).astype(wide)
    vectors = jnp.pad(vectors, ((0, 5), (0, 0)))
    routes = jnp.concatenate([route_ids.astype(wide), route_weights], axis=1)
    routes = jnp.pad(routes, ((0, 0), (0, vectors.shape[1] - routes.shape[1])))
    return jnp.concatenate([vectors, routes], axis=0)


def query_cols(me, pieces, table, weights, topk, own_rows, order, local):
    parts = len(pieces)
    cols_out, width = weights.shape
    part_rows = pieces[0].shape[0]
    part_units = part_rows // own_rows
    rows = parts * part_rows

    def kernel(me_ref, *refs):
        piece_refs = refs[:parts]
        table_ref, w_ref = refs[parts : parts + 2]
        out_refs, rows_ref = refs[parts + 2 : -1], refs[-1]
        this = me_ref[0]
        gain = table_ref[0:1, :]
        for k, ref in enumerate(piece_refs):
            for at in range(0, part_rows, 16):
                value = ref[at : at + 16, :].astype(jnp.float32)
                mean = jnp.mean(value * value, axis=-1, keepdims=True)
                normed = value * lax.rsqrt(mean + 1e-06) * gain
                base = k * part_rows + at
                rows_ref[base : base + 16, :] = normed.astype(jnp.bfloat16)
        cols = across(rows_ref[...], w_ref[...])
        routes = table_ref[8 : 8 + own_rows, 0:LANES]
        at_lane = lax.broadcasted_iota(jnp.int32, (own_rows, cols_out), 1)
        piece = (at_lane >= 2 * local).astype(jnp.int32) + (at_lane >= 4 * local).astype(jnp.int32)
        offset = (at_lane - piece * 2 * local).astype(jnp.float32)
        for s in range(parts * part_units):
            place = (this // 2) ^ (order[s] // 2)
            expert = (place * (2 * local)).astype(jnp.float32) + offset
            coeff = jnp.zeros((own_rows, cols_out), jnp.float32)
            for j in range(topk):
                weight = routes[:, topk + j : topk + j + 1]
                coeff = coeff + jnp.where(routes[:, j : j + 1] == expert, weight, 0.0)
            first = coeff.astype(jnp.bfloat16).astype(jnp.float32)
            rest = coeff - first
            second = rest.astype(jnp.bfloat16).astype(jnp.float32)
            value = jnp.where(piece == 0, first, jnp.where(piece == 1, second, rest - second))
            value = jnp.where(at_lane < 6 * local, value, 0.0)
            block = jnp.concatenate([cols[s * own_rows : (s + 1) * own_rows], value], axis=0)
            out_refs[s // part_units][s % part_units] = block.astype(jnp.bfloat16)

    shape = jax.ShapeDtypeStruct((part_units, 2 * own_rows, cols_out), jnp.bfloat16)
    return call(
        kernel,
        "query_cols",
        8,
        [SMEM_SPEC] + [VMEM_SPEC] * (parts + 2),
        [shape] * parts,
        [pltpu.VMEM((rows, width), jnp.bfloat16)],
        me,
        *pieces,
        table,
        weights,
    )


def own_token(hidden, table, w_key, w_value, w_forget, heads):
    seqs = hidden.shape[0]
    kv_heads = w_key.shape[1] // HEAD_DIM
    group = heads // kv_heads
    rows = seqs * heads

    def kernel(hid_ref, table_ref, forget_ref, key_w, value_w, out_ref):
        value = hid_ref[...].astype(jnp.float32)
        mean = jnp.mean(value * value, axis=-1, keepdims=True)
        normed = value * lax.rsqrt(mean + 1e-06) * table_ref[0:1, :]
        normed = normed.astype(jnp.bfloat16)
        gate = across(normed, forget_ref[...])
        gate = jnp.minimum(gate, 0.0) - jnp.log1p(jnp.exp(-jnp.abs(gate)))
        shape = (heads, heads)
        same = lax.broadcasted_iota(jnp.int32, shape, 0) == lax.broadcasted_iota(
            jnp.int32, shape, 1
        )
        for b in range(seqs):
            row = jnp.where(same, jnp.broadcast_to(gate[b : b + 1, :], shape), 0.0)
            total = jnp.sum(row, axis=1, keepdims=True)
            at = 2 * rows + b * heads
            out_ref[at : at + heads, :] = jnp.broadcast_to(total, (heads, HEAD_DIM))
        for weights, base in ((key_w, 0), (value_w, rows)):
            made = jnp.dot(normed, weights[...], preferred_element_type=jnp.float32)
            made = made.astype(jnp.bfloat16).astype(jnp.float32)
            for b in range(seqs):
                for g in range(kv_heads):
                    at = base + b * heads + g * group
                    part = made[b : b + 1, g * HEAD_DIM : (g + 1) * HEAD_DIM]
                    out_ref[at : at + group, :] = jnp.broadcast_to(part, (group, HEAD_DIM))

    return call(
        kernel,
        "own_token",
        8,
        [VMEM_SPEC] * 5,
        jax.ShapeDtypeStruct((3 * rows, HEAD_DIM), jnp.float32),
        [],
        hidden,
        table,
        w_forget,
        w_key,
        w_value,
    )


def attention(me, got, order, own, lengths, gate_totals, key_cache, value_cache):
    seqs, slots, width = key_cache.shape
    parts = len(got)
    part_units = got[0].shape[0]
    heads = parts * part_units
    rows = seqs * heads
    kv_heads = width // HEAD_DIM
    group = heads // kv_heads
    scale = HEAD_DIM ** (-0.5)

    def kernel(
        me_ref,
        len_ref,
        own_ref,
        gates_all,
        keys,
        values,
        *refs,
    ):
        got_refs, out_ref = refs[:parts], refs[parts]
        asked, scores, probs, mixed_ref = refs[parts + 1 :]
        for j, ref in enumerate(got_refs):
            for i in range(part_units):
                head = (me_ref[0] // 2) ^ (order[i * parts + j] // 2)
                at = pl.multiple_of(head * seqs, seqs)
                asked[pl.ds(at, seqs), :] = ref[i].astype(jnp.float32)[0:seqs]
        owner = lax.broadcasted_iota(jnp.int32, (heads, HEAD_DIM), 0) // group
        own_scores = []
        for b in range(seqs):
            at = slice(b * heads, (b + 1) * heads)
            wide = asked[pl.ds(b, heads, stride=seqs), :]
            own_scores.append(jnp.sum(wide * own_ref[at, :], axis=1, keepdims=True) * scale)
            split = jnp.concatenate(
                [jnp.where(owner == g, wide, 0.0) for g in range(kv_heads)], axis=1
            ).astype(jnp.bfloat16)
            scores[at, :] = across(split, keys[b])
        for b in range(seqs):
            at = slice(b * heads, (b + 1) * heads)
            length = len_ref[b]
            position = lax.broadcasted_iota(jnp.int32, (heads, slots), 1)
            gates = gates_all[b]
            newest = jnp.sum(
                jnp.where(position == length - 1, gates, 0.0), axis=1, keepdims=True
            )
            shift = own_ref[2 * rows + b * heads : 2 * rows + (b + 1) * heads, 0:1] + newest
            score = scores[at, :] * scale + shift - gates
            score = jnp.where(position < length, score, -jnp.inf)
            own = own_scores[b]
            peak = jnp.maximum(jnp.max(score, axis=1, keepdims=True), own)
            raised = jnp.exp(score - peak)
            own_exp = jnp.exp(own - peak)
            total = jnp.sum(raised, axis=1, keepdims=True) + own_exp
            probs[at, :] = (raised / total).astype(jnp.bfloat16)
            own_prob = (own_exp / total).astype(jnp.bfloat16).astype(jnp.float32)
            own_value = own_ref[rows + b * heads : rows + (b + 1) * heads, :]
            mixed_ref[at, :] = own_prob * own_value
        for b in range(seqs):
            at = slice(b * heads, (b + 1) * heads)
            mixed = jnp.dot(probs[at, :], values[b], preferred_element_type=jnp.float32)
            for g in range(kv_heads):
                part = slice(g * group, (g + 1) * group)
                here = slice(b * heads + g * group, b * heads + (g + 1) * group)
                mixed_ref[here, :] += mixed[part, g * HEAD_DIM : (g + 1) * HEAD_DIM]
        for h in range(heads):
            head = mixed_ref[pl.ds(h, seqs, stride=heads), :]
            out_ref[:, h * HEAD_DIM : (h + 1) * HEAD_DIM] = head.astype(jnp.bfloat16)

    return call(
        kernel,
        "attention",
        16,
        [SMEM_SPEC] * 2 + [VMEM_SPEC] * (4 + parts),
        jax.ShapeDtypeStruct((seqs, heads * HEAD_DIM), jnp.bfloat16),
        [
            pltpu.VMEM((rows, HEAD_DIM), jnp.float32),
            pltpu.VMEM((rows, slots), jnp.float32),
            pltpu.VMEM((rows, slots), jnp.bfloat16),
            pltpu.VMEM((rows, HEAD_DIM), jnp.float32),
        ],
        me,
        lengths,
        own,
        gate_totals,
        key_cache,
        value_cache,
        *got,
    )


def resid_cols(me, pieces, hidden, weights):
    parts = len(pieces)
    part_rows, width = pieces[0].shape
    cols_out = weights.shape[0]

    def kernel(me_ref, *refs):
        row_refs, hid_refs = refs[:parts], refs[parts : 2 * parts]
        w_ref, out_ref, rows_ref = refs[2 * parts :]
        for k, ref in enumerate(row_refs):
            rows_ref[k * part_rows : (k + 1) * part_rows, :] = ref[...]
        made = across(rows_ref[...], w_ref[...]).astype(jnp.bfloat16).astype(jnp.float32)
        col = pl.multiple_of(me_ref[0] // 2 * cols_out, cols_out)
        for k, ref in enumerate(hid_refs):
            at = slice(k * part_rows, (k + 1) * part_rows)
            held = ref[:, pl.ds(col, cols_out)].astype(jnp.float32)
            out_ref[at, :] = (held + made[at]).astype(jnp.bfloat16)

    rows = parts * part_rows
    return call(
        kernel,
        "resid_cols",
        8,
        [SMEM_SPEC] + [VMEM_SPEC] * (2 * parts + 1),
        jax.ShapeDtypeStruct((rows, cols_out), jnp.bfloat16),
        [pltpu.VMEM((rows, width), jnp.bfloat16)],
        me,
        *pieces,
        *hidden,
        weights,
    )


def mix(me, blocks, table, got, weights, order, own_rows):
    parts = len(blocks)
    unit = own_rows
    rows = len(order) * unit
    width = table.shape[1]
    lane_rows = rows // 2
    part_units = len(order) // parts
    half = len(order) // 2
    got_parts = len(got) // 2
    dense_ff = weights[0].shape[1]
    local, _, exp_ff = weights[2].shape

    def kernel(me_ref, *refs):
        block_refs, refs = refs[:parts], refs[parts:]
        table_ref, got_refs = refs[0], refs[1 : 1 + len(got)]
        refs = refs[1 + len(got) :]
        dense_gate, dense_up, exp_gate, exp_up, dense_down, exp_down = refs[:6]
        near_ref, far_ref, resid_ref, normed_ref = refs[6:10]
        resid_all, rows_ref, blend_ref, coeff_ref, act_ref = refs[10:15]
        this = me_ref[0]
        for p in range(parts * part_units):
            ref = block_refs[p // part_units]
            base = p % part_units * lane_rows
            col = pl.multiple_of(((this // 2) ^ (order[p] // 2)) * LANES, LANES)
            for s in range(0, lane_rows // unit, 2):
                pair = ref[base + s * unit : base + (s + 2) * unit, :].astype(jnp.float32)
                for u in range(2):
                    row = (p ^ (s + u)) * unit
                    resid_all[row : row + unit, pl.ds(col, LANES)] = pair[
                        u * unit : (u + 1) * unit
                    ]
        at_lane = lax.broadcasted_iota(jnp.int32, (unit, LANES), 1)
        for j in range(local):
            wanted = this % 2 * local + j
            chosen = (at_lane == wanted) | (at_lane == wanted + 2 * local)
            chosen = chosen | (at_lane == wanted + 4 * local)
            for p in range(parts * part_units):
                source = got_refs[p // half * got_parts + p % got_parts]
                block = source[p % half // got_parts].astype(jnp.float32)
                picked = jnp.where(chosen, block[unit:], 0.0)
                total = jnp.sum(picked, axis=1, keepdims=True)
                coeff_ref[j, p * unit : (p + 1) * unit, :] = jnp.broadcast_to(
                    total, (unit, LANES)
                )
        gain = table_ref[1:2, :]
        blend_w = table_ref[2:3, :]
        for at in range(0, rows, 16):
            here = slice(at, at + 16)
            resid = resid_all[here, :]
            if at == 0:
                resid_ref[...] = resid[:unit].astype(jnp.bfloat16)
            mean = jnp.mean(resid * resid, axis=-1, keepdims=True)
            normed = (resid * lax.rsqrt(mean + 1e-06) * gain).astype(jnp.bfloat16)
            rows_ref[here, :] = normed
            score = jnp.sum(normed.astype(jnp.float32) * blend_w, axis=-1, keepdims=True)
            blend_ref[here, :] = jnp.broadcast_to(jax.nn.sigmoid(score), (16, LANES))
        normed_ref[...] = rows_ref[0:unit, :]
        all_rows = rows_ref[...]
        gate = jnp.dot(all_rows, dense_gate[...], preferred_element_type=jnp.float32)
        up = jnp.dot(all_rows, dense_up[...], preferred_element_type=jnp.float32)
        act = jax.nn.silu(gate) * up * blend_ref[:, 0:1]
        act_ref[:, 0:dense_ff] = act.astype(jnp.bfloat16)
        for j in range(local):
            for start in range(0, exp_ff, 256):
                cols = slice(start, min(start + 256, exp_ff))
                gate = jnp.dot(all_rows, exp_gate[j, :, cols], preferred_element_type=jnp.float32)
                up = jnp.dot(all_rows, exp_up[j, :, cols], preferred_element_type=jnp.float32)
                act = jax.nn.silu(gate) * up * coeff_ref[j, :, 0:1]
                base = dense_ff + j * exp_ff
                act_ref[:, base + cols.start : base + cols.stop] = act.astype(jnp.bfloat16)
        for start in range(0, width, 512):
            cols = slice(start, min(start + 512, width))
            total = jnp.dot(
                act_ref[:, 0:dense_ff], dense_down[:, cols], preferred_element_type=jnp.float32
            )
            for j in range(local):
                base = dense_ff + j * exp_ff
                total = total + jnp.dot(
                    act_ref[:, base : base + exp_ff],
                    exp_down[j, :, cols],
                    preferred_element_type=jnp.float32,
                )
            near_ref[:, cols] = total[:lane_rows].astype(jnp.bfloat16)
            far_ref[:, cols] = total[lane_rows:].astype(jnp.bfloat16)

    ff_total = dense_ff + local * exp_ff
    narrow = jnp.bfloat16
    return call(
        kernel,
        "mix",
        24,
        [SMEM_SPEC] + [VMEM_SPEC] * (parts + 7 + len(got)),
        [
            jax.ShapeDtypeStruct((lane_rows, width), narrow),
            jax.ShapeDtypeStruct((lane_rows, width), narrow),
            jax.ShapeDtypeStruct((unit, width), narrow),
            jax.ShapeDtypeStruct((unit, width), narrow),
        ],
        [
            pltpu.VMEM((rows, width), jnp.float32),
            pltpu.VMEM((rows, width), narrow),
            pltpu.VMEM((rows, LANES), jnp.float32),
            pltpu.VMEM((local, rows, LANES), jnp.float32),
            pltpu.VMEM((rows, ff_total), narrow),
        ],
        me,
        *blocks,
        table,
        *got,
        *weights,
    )


def make_body(mesh):
    count = mesh.shape[AXIS]
    groups = stages_of(mesh)
    order = jnp.array(block_order(groups), jnp.int32)

    def on_device(
        hidden_in,
        w_query,
        w_key,
        w_value,
        w_forget,
        w_out,
        attn_gain,
        key_cache,
        value_cache,
        gate_totals,
        lengths,
        mix_gain,
        route_ids,
        route_weights,
        exp_gate,
        exp_up,
        exp_down,
        shared_gate,
        shared_up,
        shared_down,
        dense_gate,
        dense_up,
        dense_down,
        blend_weight,
    ):
        me = lax.axis_index(AXIS)
        own_rows, width = hidden_in.shape
        rows = own_rows * count
        topk = route_ids.shape[1]
        source = jnp.repeat(order ^ me, own_rows) * own_rows + jnp.tile(
            jnp.arange(own_rows, dtype=jnp.int32), count
        )
        to_device = (jnp.arange(rows, dtype=jnp.int32)[:, None] == source[None, :]).astype(
            jnp.bfloat16
        )

        def columns_of(all_rows, weights):
            cols = jnp.dot(all_rows, weights, preferred_element_type=jnp.float32)
            cols = cols.astype(jnp.bfloat16)
            sorted_cols = jnp.dot(to_device, cols, preferred_element_type=jnp.float32)
            return lax.all_to_all(
                sorted_cols.astype(jnp.bfloat16), AXIS, split_axis=0, concat_axis=1, tiled=True
            )

        normed = normalize(hidden_in, attn_gain)
        packed = pack_routes(route_ids, route_weights, 128)
        first = gather_rows(jnp.concatenate([normed, packed], axis=1), groups, count)
        ids, weights = unpack_routes(first[:, width:], topk)
        queries = columns_of(first[:, :width], w_query)
        new_key = jnp.dot(normed, w_key, preferred_element_type=jnp.float32).astype(jnp.bfloat16)
        new_value = jnp.dot(normed, w_value, preferred_element_type=jnp.float32).astype(
            jnp.bfloat16
        )
        forget = jax.nn.log_sigmoid(jnp.dot(normed, w_forget, preferred_element_type=jnp.float32))
        mixture = attend(
            queries, new_key, new_value, forget, key_cache, value_cache, gate_totals, lengths
        )
        attn_out = columns_of(gather_rows(mixture, groups, count), w_out)
        resid = (hidden_in.astype(jnp.float32) + attn_out.astype(jnp.float32)).astype(jnp.bfloat16)
        normed2 = normalize(resid, mix_gain)
        all_rows = gather_rows(normed2, groups, count)

        local = exp_gate.shape[0]
        blend = jax.nn.sigmoid(jnp.dot(all_rows, blend_weight, preferred_element_type=jnp.float32))
        dense_hidden = (
            jax.nn.silu(jnp.dot(all_rows, dense_gate, preferred_element_type=jnp.float32))
            * jnp.dot(all_rows, dense_up, preferred_element_type=jnp.float32)
            * blend[:, None]
        ).astype(jnp.bfloat16)
        partial = jnp.dot(dense_hidden, dense_down, preferred_element_type=jnp.float32)
        for j in range(local):
            coeff = jnp.sum(jnp.where(ids == me * local + j, weights, 0.0), axis=1)
            expert_hidden = (
                jax.nn.silu(jnp.dot(all_rows, exp_gate[j], preferred_element_type=jnp.float32))
                * jnp.dot(all_rows, exp_up[j], preferred_element_type=jnp.float32)
                * coeff[:, None]
            ).astype(jnp.bfloat16)
            partial = partial + jnp.dot(
                expert_hidden, exp_down[j], preferred_element_type=jnp.float32
            )
        branch = scatter_sum(partial, groups, count)
        shared_hidden = (
            jax.nn.silu(jnp.dot(normed2, shared_gate, preferred_element_type=jnp.float32))
            * jnp.dot(normed2, shared_up, preferred_element_type=jnp.float32)
        ).astype(jnp.bfloat16)
        shared_out = jnp.dot(shared_hidden, shared_down, preferred_element_type=jnp.float32)
        return (resid.astype(jnp.float32) + shared_out + branch).astype(jnp.bfloat16)

    first_masks = groups[0]
    mid_masks = block_order(groups[1:-1])[1:]
    wide_groups = [first_masks, mid_masks, [1]]
    positions = block_order(wide_groups)

    def gather_lane(rows):
        line = join_rows([rows] + [swap(rows, mask, count) for mask in first_masks])
        return [line] + [swap(line, mask, count) for mask in mid_masks]

    def fast_path(
        hidden_in,
        w_query,
        w_key,
        w_value,
        w_forget,
        w_out,
        attn_gain,
        key_cache,
        value_cache,
        gate_totals,
        lengths,
        mix_gain,
        route_ids,
        route_weights,
        exp_gate,
        exp_up,
        exp_down,
        shared_gate,
        shared_up,
        shared_down,
        dense_gate,
        dense_up,
        dense_down,
        blend_weight,
    ):
        me = lax.axis_index(AXIS)
        this = me.astype(jnp.int32).reshape(1)
        own_rows, width = hidden_in.shape
        heads = gate_totals.shape[1]
        local = exp_gate.shape[0]

        hid_line = join_rows(
            [join_rows([hidden_in])] + [swap(hidden_in, mask, count) for mask in first_masks]
        )
        hid_lane = [hid_line] + [swap(hid_line, mask, count) for mask in mid_masks]
        wq_own, wo_own = w_query.T, w_out.T
        wq_pair = chip_weights(this, wq_own, swap(wq_own, 1, count))
        table = small_table(attn_gain, mix_gain, blend_weight, route_ids, route_weights)
        sent = query_cols(
            this, hid_lane, table, wq_pair, route_ids.shape[1], own_rows, positions, local
        )
        hidden_late, wo_late, _ = lax.optimization_barrier((hidden_in, wo_own, hid_line))
        own = own_token(hidden_late, table, w_key, w_value, w_forget.T, heads)
        crossed = sent[:1] + [
            swap(piece, mask, count) for piece, mask in zip(sent[1:], mid_masks)
        ]
        crossed = regroup(crossed)
        got = crossed[:1] + [
            swap(piece, mask, count) for piece, mask in zip(crossed[1:], first_masks)
        ]
        mixture = attention(
            this, got, positions, own, lengths, gate_totals, key_cache, value_cache
        )
        wo_pair = chip_weights(this, wo_late, swap(wo_late, 1, count))
        resid_block = resid_cols(this, gather_lane(mixture), hid_lane, wo_pair)
        blocks = gather_lane(resid_block)
        blocks = blocks + [swap(piece, 1, count) for piece in blocks]
        got_late, _ = lax.optimization_barrier((got, mixture))
        got = got + [swap(piece, 1, count) for piece in got_late]
        near, far, resid, normed2 = mix(
            this,
            blocks,
            table,
            got,
            (dense_gate, dense_up, exp_gate, exp_up, dense_down, exp_down),
            positions,
            own_rows,
        )
        near = near.astype(jnp.float32) + swap(far, 1, count).astype(jnp.float32)
        branch = scatter_sum(near, [first_masks, mid_masks], count)
        shared_hidden = (
            jax.nn.silu(jnp.dot(normed2, shared_gate, preferred_element_type=jnp.float32))
            * jnp.dot(normed2, shared_up, preferred_element_type=jnp.float32)
        ).astype(jnp.bfloat16)
        shared_out = jnp.dot(shared_hidden, shared_down, preferred_element_type=jnp.float32)
        kept = lax.optimization_barrier(resid.astype(jnp.float32) + shared_out)
        return (kept + branch).astype(jnp.bfloat16)

    def choose(*args):
        own_rows, width = args[0].shape
        cols = args[1].shape[1]
        slots_width = args[7].shape[2]
        linear = len(groups) > 2 and all(
            positions[p ^ s] == positions[p] ^ positions[s]
            for p in range(count)
            for s in range(count)
        )
        if (
            linear
            and groups[-1] == [1]
            and own_rows == 8
            and 2 * cols == HEAD_DIM
            and args[5].shape[1] == cols
            and slots_width % HEAD_DIM == 0
            and 6 * args[14].shape[0] <= 2 * cols
        ):
            return fast_path(*args)
        return on_device(*args)

    return choose


def solution(mesh):
    row, col, cube, whole = P(AXIS, None), P(None, AXIS), P(AXIS, None, None), P()
    placed = (
        row,
        col,
        whole,
        whole,
        whole,
        col,
        whole,
        cube,
        cube,
        cube,
        P(AXIS),
        whole,
        row,
        row,
        cube,
        cube,
        cube,
        whole,
        whole,
        whole,
        col,
        col,
        row,
        whole,
    )
    return jax.shard_map(
        make_body(mesh), mesh=mesh, in_specs=placed, out_specs=row, check_vma=False
    )
```
